256 devices in a mesh: grp: 2 (over y), sp: 32 (over z, core), tp: 4 (over x).
Axes of the slice: x: 4, y: 2, z: 16, core: 2. Of those that a mesh axis runs over, the one named last changes fastest.
The devices are a block of a 4x16x16 slice.
Arguments:
- stream: bfloat16 [16384, 4096], P(('grp', 'sp'), 'tp'), parts along dimension 0, may hold values from -6 to 6
- gain_pre: float32 [3, 4096], replicated, may hold values from 0.1 to 1.9
- w_in: bfloat16 [3, 4096, 1024], P(None, 'sp', 'tp'), may hold values from -0.09375 to 0.09375
- w_pool: bfloat16 [3, 4, 256, 256], P(None, 'tp'), may hold values from -0.375 to 0.375
- pool_scale: float32 [3, 1024], P(None, 'tp'), may hold values from 0.1 to 1.9
- w_out: bfloat16 [3, 1024, 4096], P(None, 'tp', 'sp'), may hold values from -0.5 to 0.5
- gain_post: float32 [3, 4096], replicated, may hold values from 0.1 to 1.9
Outputs:
- result: bfloat16 [16384, 4096], P(('grp', 'sp'), 'tp'), parts along dimension 0
The draws below stay inside these ranges and needn't reach their ends.
There are 2 independent parts, one for each index of `grp`. The reference program is written for one: setup_inputs(seed, part) draws one part's arguments, and reference() takes and returns one part's arrays. A program takes and returns all parts, laid end to end along the dimension named above; an argument that names none is the same for every part. Nothing has to cross between parts.
All inputs are finite; a program needn't handle non-finite values.
Results may differ from the reference program's by a relative error of at most 0.02.
Values may be sent and summed in bfloat16 or wider, within the bound.
A program may use at most 64 MiB of HBM per device.

```python
import jax
import jax.numpy as jnp
from jax import lax

D = 4096
GROUP = 256
POOL = 1024
LAYERS = 3
TOKENS = 8192


def draw_w_out(key, part):
    key_entries = jax.random.fold_in(key, 11)
    key_rough = jax.random.fold_in(key, 12)
    column_place = jnp.arange(D).astype(jnp.float32) / float(D - 1)
    rough = jax.random.uniform(key_rough, (D,), jnp.float32, 0.7, 1.4)
    entries = jax.random.normal(key_entries, (LAYERS, POOL, D), jnp.float32)
    column_scale = 0.4 * jnp.exp(jnp.log(6.0) * column_place) * rough
    values = entries * column_scale[None, None, :] * float(POOL) ** (-0.5)
    values = jnp.clip(values, -0.5, 0.5)
    return values.astype(jnp.bfloat16)


def block_levels(key, shape, pieces, low, high):
    level = 1.0
    for dim, parts in pieces:
        steps = jax.random.uniform(jax.random.fold_in(jax.random.fold_in(key, 6), dim), (parts,), jnp.float32, low / len(pieces), high / len(pieces))
        level = level * jnp.repeat(jnp.exp(steps), shape[dim] // parts).reshape((-1,) + (1,) * (len(shape) - 1 - dim))
    return level


def gaussian(rng, extent, deviation, most, shards=(), dtype=jnp.bfloat16):
    factor_of = block_levels(rng, extent, shards, -0.22, 0.18) if shards else 1.0
    values = jax.random.normal(rng, extent, jnp.float32) * deviation * factor_of
    return jnp.minimum(jnp.maximum(values, -most), most).astype(dtype)


def setup_inputs(seed: int = 0, part: int = 0) -> dict:
    arg_keys = jax.random.split(jax.random.key(seed), 8)
    part_keys = jax.random.split(jax.random.fold_in(arg_keys[7], part), 8)
    return {
        "stream": gaussian(part_keys[0], (TOKENS, D), 1.0, 6.0, ((0, 32), (1, 4))),
        "gain_pre": jnp.clip(1.0 + 0.18 * jax.random.normal(arg_keys[1], (LAYERS, D), jnp.float32), 0.1, 1.9),
        "w_in": gaussian(arg_keys[2], (LAYERS, D, POOL), D ** -0.5, 0.09375, ((1, 32), (2, 4))),
        "w_pool": gaussian(arg_keys[3], (LAYERS, 4, GROUP, GROUP), GROUP ** -0.5, 0.375, ((1, 4),)),
        "pool_scale": jnp.clip(1.0 + 0.18 * jax.random.normal(arg_keys[4], (LAYERS, POOL), jnp.float32), 0.1, 1.9),
        "w_out": draw_w_out(jax.random.fold_in(arg_keys[7], 71), part),
        "gain_post": jnp.clip(1.0 + 0.18 * jax.random.normal(arg_keys[6], (LAYERS, D), jnp.float32), 0.1, 1.9),
    }


WINDOWS = (2, 4, 8, 16)
EPS = 1e-06

def rms_scale(values, gain):
    inverse = lax.rsqrt(lax.optimization_barrier(jnp.mean(values * values, axis=-1, keepdims=True)) + EPS)
    return values * inverse * gain[None, :]

def reference(stream, gain_pre, w_in, w_pool, pool_scale, w_out, gain_post):
    reach = max(WINDOWS) - 1
    positions = jnp.arange(TOKENS).astype(jnp.float32)
    current = stream
    for layer in range(LAYERS):
        normed = rms_scale(current.astype(jnp.float32), gain_pre[layer]).astype(jnp.bfloat16)
        inner = jnp.dot(normed, w_in[layer], preferred_element_type=jnp.float32).astype(jnp.bfloat16)
        inner_f = inner.astype(jnp.float32)
        padded = jnp.concatenate([jnp.zeros((reach, 4 * GROUP), jnp.float32), inner_f], axis=0)
        branch = jnp.zeros((TOKENS, D), jnp.float32)
        for group_id in range(4):
            window = WINDOWS[group_id]
            lo = group_id * GROUP
            summed = jnp.zeros((TOKENS, GROUP), jnp.float32)
            for offset in range(window):
                summed = summed + padded[reach - offset:reach - offset + TOKENS, lo:lo + GROUP]
            count = jnp.minimum(positions + 1.0, float(window))
            pooled = summed / count[:, None]
            spread = (pooled - inner_f[:, lo:lo + GROUP]).astype(jnp.bfloat16)
            mixed = jnp.dot(spread, w_pool[layer, group_id], preferred_element_type=jnp.float32)
            mixed = (mixed * pool_scale[layer, lo:lo + GROUP][None, :]).astype(jnp.bfloat16)
            partial_value = jnp.dot(mixed, w_out[layer, lo:lo + GROUP], preferred_element_type=jnp.float32)
            partial_value = lax.optimization_barrier(partial_value.astype(jnp.bfloat16))
            branch = branch + partial_value.astype(jnp.float32)
        current = (current.astype(jnp.float32) + rms_scale(branch, gain_post[layer])).astype(jnp.bfloat16)
    return current
```

```python
import functools

import jax
import jax.numpy as jnp
from jax import lax
from jax.experimental import pallas as pl
from jax.experimental.pallas import tpu as pltpu
from jax.sharding import PartitionSpec as P

EPS = 1e-06
HALO = 16
LANES = 128
CHUNK = 32
MESH = pl.DeviceIdType.MESH
F32 = jnp.float32
BF16 = jnp.bfloat16

A = [[(1, j), (2, j)] for j in range(8)]
B = [[(3, j), (4, j)] for j in range(8)]
C = [[(5, j)] for j in range(8)]
PLACES = {
    "start": [[(0, j)] for j in range(5)]
    + [[(0, 5)] + A[0], [(0, 6)] + A[1], [(0, 7)] + A[2]],
    ("halo", 0): A[3:4],
    ("mix", 0): A[4:8],
    ("square", 0): B[0:1],
    ("sum", 1): B[1:4],
    ("halo", 1): [B[4] + C[0]],
    ("mix", 1): [B[5] + C[1], B[6] + C[2], B[7] + C[3]],
    ("square", 1): C[4:5],
    ("sum", 2): C[5:7],
    ("halo", 2): C[7:8],
    ("mix", 2): [],
}


def kernel(
    n_sp, n_tp,
    stream, gain_pre, w_in, w_pool, pool_scale, w_out, gain_post, out,
    full, lhs0, win0, win, wout, lhs, cur, branch, own_y, rs_out, rs_in, mix, rows_acc,
    ss_out, ss_in, edge_out, edge_in, ext,
    ring_recv, part_recv, ring_send, swap_send, swap_recv, local_sem,
    x_send, x_recv, rs_send, rs_recv, ss_send, ss_recv, mix_send, mix_recv, edge_send, edge_recv,
):
    s = lax.axis_index("sp")
    t = lax.axis_index("tp")
    layers = w_in.shape[0]
    depth = w_in.shape[1]
    group = w_in.shape[2]
    tok, block = stream.shape
    width = gain_pre.shape[1]
    half = tok // 2
    chips = n_sp // 2
    plus = chips // 2
    minus = chips - 1 - plus
    span = n_sp // n_tp
    mats = 2 * layers
    quarter, rest = lax.div(s, span), lax.rem(s, span)
    home = {"sp": t * span + rest, "tp": quarter}
    stays = quarter == t
    moves = quarter != t
    up = {"sp": lax.rem(s + 2, n_sp)}
    down = {"sp": lax.rem(s + n_sp - 2, n_sp)}
    partner = {"sp": s + 1 - 2 * lax.rem(s, 2)}
    after = {"sp": lax.rem(s + 1, n_sp)}
    before = {"sp": lax.rem(s + n_sp - 1, n_sp)}
    tps = [lax.rem(t + k, n_tp) for k in range(n_tp)]

    def remote(src, dst, send, recv, device):
        copy = pltpu.make_async_remote_copy(
            src_ref=src, dst_ref=dst, send_sem=send, recv_sem=recv,
            device_id=device, device_id_type=MESH,
        )
        copy.start()
        return copy

    def arrived(ref, sem):
        pltpu.make_async_copy(ref, ref, sem).wait()

    barrier = pltpu.get_barrier_semaphore()
    greeted = [up, down, before, after] + [{"tp": k} for k in tps[1:]]
    for device in greeted:
        pl.semaphore_signal(barrier, inc=1, device_id=device, device_id_type=MESH)

    @pl.when(moves)
    def _():
        pl.semaphore_signal(barrier, inc=1, device_id=home, device_id_type=MESH)

    pl.semaphore_wait(barrier, len(greeted) + jnp.where(moves, 1, 0))

    def slot(m, src):
        if m % 2 == 0:
            rows = pl.ds(pl.multiple_of(src * depth, depth), depth)
            return win0.at[rows] if m == 0 else win.at[m // 2 - 1, rows]
        rows = pl.ds(pl.multiple_of(lax.div(src, span) * group, group), group)
        columns = pl.ds(pl.multiple_of(lax.rem(src, span) * depth, depth), depth)
        return wout.at[m // 2, rows, columns]

    def pieces(m, count):
        if m % 2 == 0:
            rows = pl.ds(0, count * depth)
            return win0.at[rows] if m == 0 else win.at[m // 2 - 1, rows]
        unit = group * depth // block
        return wout.at[m // 2, pl.ds(0, count * unit)]

    def original(m):
        return w_in.at[m // 2] if m % 2 == 0 else w_out.at[m // 2]

    def spread_own(m):
        src = slot(m, s) if m else original(0)
        remote(src, slot(m, s), ring_send.at[m], ring_recv.at[m, 0, 0], up)
        remote(src, slot(m, s), ring_send.at[m], ring_recv.at[m, 1, 0], down)
        remote(src, slot(m, s), ring_send.at[m], part_recv.at[m], partner)

    def swap_started(m):
        here = home["sp"]

        @pl.when(moves)
        def _():
            remote(original(m), slot(m, s_of_home(m)), swap_send.at[m], swap_recv.at[m], home)

        @pl.when(stays)
        def _():
            pltpu.make_async_copy(original(m), slot(m, s), swap_recv.at[m]).start()

    def s_of_home(m):
        return home["sp"]

    def swap_ended(m):
        arrived(slot(m, s), swap_recv.at[m])

    def step(m, j):
        if j == 0 and m > 0:
            swap_ended(m)
            spread_own(m)
        for way, reach, device in ((0, plus, up), (1, minus, down)):
            if j >= reach:
                continue
            distance = 2 * (j + 1)
            src = lax.rem(s + n_sp - distance if way == 0 else s + distance, n_sp)
            piece = slot(m, src)
            arrived(piece, ring_recv.at[m, way, j])
            if j + 1 < reach:
                remote(piece, piece, ring_send.at[m], ring_recv.at[m, way, j + 1], device)
            remote(piece, piece, ring_send.at[m], part_recv.at[m], partner)

    def ticks(place):
        for tick in PLACES.get(place, []):
            for m, j in tick:
                step(m, j)

    def whole(m):
        arrived(pieces(m, chips), part_recv.at[m])

    lo, hi = pl.ds(0, half), pl.ds(half, half)
    spread_own(0)
    mine = full.at[t]
    right, left = {"tp": tps[1]}, {"tp": tps[n_tp - 1]}
    remote(stream.at[lo], mine.at[lo], x_send.at[0], x_recv.at[0], right)
    remote(stream.at[hi], mine.at[hi], x_send.at[1], x_recv.at[1], left)
    swap_started(1)
    remote(stream.at[hi], mine.at[hi], x_send.at[2], x_recv.at[2], right)
    remote(stream.at[lo], mine.at[lo], x_send.at[3], x_recv.at[3], left)
    own_rows = pltpu.make_async_copy(stream, mine, local_sem.at[0])
    own_rows.start()
    own_piece = pltpu.make_async_copy(original(0), slot(0, s), local_sem.at[1])
    own_piece.start()
    for m in range(2, mats):
        swap_started(m)

    def squares(x):
        total = x[:, :LANES] * x[:, :LANES]
        for k in range(1, x.shape[1] // LANES):
            part = x[:, k * LANES:(k + 1) * LANES]
            total = total + part * part
        return total

    def prepare(b, first):
        gain = gain_pre[0:1, pl.ds(pl.multiple_of(b * block, block), block)]

        @pl.loop(0, tok // CHUNK)
        def _(i):
            rows = pl.ds(pl.multiple_of(i * CHUNK, CHUNK), CHUNK)
            x = full[b, rows, :].astype(F32)
            lhs0[b, rows, :] = (x * gain).astype(BF16)
            sums = squares(x)
            rows_acc[rows, :] = sums if first else rows_acc[rows, :] + sums

    start = PLACES["start"]

    def start_tick(i):
        for m, j in start[i]:
            step(m, j)

    start_tick(0)
    own_rows.wait()
    prepare(t, True)
    start_tick(1)
    behind, ahead, across = full.at[tps[n_tp - 1]], full.at[tps[1]], full.at[tps[2]]
    arrived(behind.at[lo], x_recv.at[0])
    remote(behind.at[lo], behind.at[lo], x_send.at[4], x_recv.at[4], right)
    arrived(ahead.at[hi], x_recv.at[1])
    remote(ahead.at[hi], ahead.at[hi], x_send.at[5], x_recv.at[5], left)
    start_tick(2)
    start_tick(3)
    arrived(behind.at[hi], x_recv.at[2])
    arrived(ahead.at[lo], x_recv.at[3])
    prepare(tps[n_tp - 1], False)
    start_tick(4)
    prepare(tps[1], False)
    start_tick(5)
    arrived(across.at[lo], x_recv.at[4])
    arrived(across.at[hi], x_recv.at[5])
    start_tick(6)
    prepare(tps[2], False)
    start_tick(7)
    own_piece.wait()
    whole(0)

    def row_of(acc):
        return jnp.broadcast_to(jnp.sum(acc.T, axis=0, keepdims=True), (8, tok))

    def inverse(row):
        inv = lax.rsqrt(row / width + EPS)
        return jnp.concatenate([inv] * (LANES // 8), axis=0).T

    def across_lanes(column, lanes):
        return jnp.concatenate([column] * (lanes // LANES), axis=1)

    def send_squares(kind, row):
        ss_out[kind] = row
        for k in range(1, n_tp):
            remote(
                ss_out.at[kind], ss_in.at[kind, k], ss_send.at[kind, k], ss_recv.at[kind, k],
                {"tp": tps[k]},
            )

    def sum_squares(kind):
        total = ss_out[kind]
        for k in range(1, n_tp):
            arrived(ss_in.at[kind, k], ss_recv.at[kind, k])
            total = total + ss_in[kind, k]
        return total

    position = s * tok + lax.broadcasted_iota(jnp.int32, (tok, LANES), 0)
    window = 2
    for k in range(1, n_tp):
        window = jnp.where(t == k, 2 << k, window)
    count = jnp.minimum(position + 1, window).astype(F32)

    for l in range(layers):
        if l == 0:
            acc = jnp.dot(lhs0[0], win0[0:block, :], preferred_element_type=F32)
            for b in range(1, n_tp):
                acc = acc + jnp.dot(
                    lhs0[b], win0[b * block:(b + 1) * block, :], preferred_element_type=F32
                )
            inv = inverse(row_of(rows_acc[...]))
        else:
            whole(2 * l)
            for k in (2, 1, 3, 0):
                first = pl.multiple_of(tps[k] * block, block)
                y = jnp.dot(lhs[...], win[l - 1, pl.ds(first, block), :], preferred_element_type=F32)
                if k == 0:
                    own_y[...] = y
                else:
                    rs_out[l - 1, k] = y.astype(BF16)
                    remote(
                        rs_out.at[l - 1, k], rs_in.at[l - 1, k],
                        rs_send.at[l - 1, k], rs_recv.at[l - 1, k], {"tp": tps[k]},
                    )
            ticks(("sum", l))
            inv = inverse(sum_squares(layers + l - 1))
            acc = own_y[...]
            for k in range(1, n_tp):
                arrived(rs_in.at[l - 1, k], rs_recv.at[l - 1, k])
                acc = acc + rs_in[l - 1, k].astype(F32)
        inner = (acc * across_lanes(inv, group)).astype(BF16)
        edge_out[l] = inner[tok - HALO:, :]
        remote(edge_out.at[l], edge_in.at[l], edge_send.at[l], edge_recv.at[l], after)
        inner = inner.astype(F32)
        ext[HALO:, :] = inner
        ticks(("halo", l))
        arrived(edge_in.at[l], edge_recv.at[l])
        ext[0:HALO, :] = jnp.where(s > 0, edge_in[l].astype(F32), 0.0)
        sums = ext[...]
        chosen = None
        for k in range(n_tp):
            sums = sums + pltpu.roll(sums, 1 << k, 0)
            chosen = sums if chosen is None else jnp.where(t >= k, sums, chosen)
        pooled = chosen[HALO:, :] / across_lanes(count, group)
        spread = (pooled - ext[HALO:, :]).astype(BF16)
        mixed = jnp.dot(spread, w_pool[l, 0], preferred_element_type=F32)
        mixed = (mixed * pool_scale[l:l + 1, :]).astype(BF16)
        own = pl.ds(pl.multiple_of(t * group, group), group)
        mix[l, :, own] = mixed
        place = mix.at[l, :, own]
        for k in (2, 1, 3):
            remote(place, place, mix_send.at[l, k], mix_recv.at[l, k], {"tp": tps[k]})
        ticks(("mix", l))
        for k in (1, 3, 2):
            theirs = pl.ds(pl.multiple_of(tps[(n_tp - k) % n_tp] * group, group), group)
            arrived(mix.at[l, :, theirs], mix_recv.at[l, k])
        whole(2 * l + 1)
        total = None
        for n in range(block // group):
            columns = slice(n * group, (n + 1) * group)
            y = jnp.dot(mix[l], wout[l, :, columns], preferred_element_type=F32)
            branch[:, columns] = y
            total = squares(y) if total is None else total + squares(y)
        send_squares(l, row_of(total))
        ticks(("square", l))
        rows_acc[...] = inverse(sum_squares(l))
        mine_only = pl.ds(pl.multiple_of(t * block, block), block)
        gain = gain_post[l:l + 1, mine_only]
        before_l = full.at[t] if l == 0 else cur
        if l + 1 < layers:
            next_gain = gain_pre[l + 1:l + 2, mine_only]

        @pl.loop(0, tok // CHUNK)
        def _(i):
            rows = pl.ds(pl.multiple_of(i * CHUNK, CHUNK), CHUNK)
            scale = across_lanes(rows_acc[rows, :], block)
            new = before_l[rows, :].astype(F32) + branch[rows, :] * scale * gain
            new = new.astype(BF16)
            if l + 1 < layers:
                cur[rows, :] = new
                new = new.astype(F32)
                lhs[rows, :] = (new * next_gain).astype(BF16)
                rows_acc[rows, :] = squares(new)
            else:
                out[rows, :] = new

        if l + 1 < layers:
            send_squares(layers + l, row_of(rows_acc[...]))

    for m in range(mats):
        arrived(pieces(m, plus + minus + chips), ring_send.at[m])
        if m:
            @pl.when(moves)
            def _():
                arrived(slot(m, s), swap_send.at[m])
    for k in range(6):
        arrived(mine.at[lo], x_send.at[k])
    for l in range(layers):
        arrived(edge_out.at[l], edge_send.at[l])
        for k in range(1, n_tp):
            arrived(mix.at[l, :, pl.ds(0, group)], mix_send.at[l, k])
            arrived(ss_out.at[l], ss_send.at[l, k])
            if l:
                arrived(rs_out.at[l - 1, k], rs_send.at[l - 1, k])
                arrived(ss_out.at[l], ss_send.at[layers + l - 1, k])


def solution(mesh):
    n_sp, n_tp = mesh.shape["sp"], mesh.shape["tp"]

    def per_device(stream, gain_pre, w_in, w_pool, pool_scale, w_out, gain_post):
        tok, block = stream.shape
        layers, depth, group = w_in.shape
        width = gain_pre.shape[1]
        channels = n_tp * group
        mats = 2 * layers
        kinds = 2 * layers - 1
        reach = n_sp // 4
        dma = pltpu.SemaphoreType.DMA
        vmem = pl.BlockSpec(memory_space=pltpu.VMEM)
        hbm = pl.BlockSpec(memory_space=pl.ANY)
        return pl.pallas_call(
            functools.partial(kernel, n_sp, n_tp),
            out_shape=jax.ShapeDtypeStruct((tok, block), BF16),
            in_specs=[hbm, vmem, hbm, vmem, vmem, hbm, vmem],
            out_specs=vmem,
            scratch_shapes=[
                pltpu.VMEM((n_tp, tok, block), BF16),
                pltpu.VMEM((n_tp, tok, block), BF16),
                pltpu.VMEM((width, group), BF16),
                pltpu.VMEM((layers - 1, n_tp * block, group), BF16),
                pltpu.VMEM((layers, channels, block), BF16),
                pltpu.VMEM((tok, block), BF16),
                pltpu.VMEM((tok, block), BF16),
                pltpu.VMEM((tok, block), F32),
                pltpu.VMEM((tok, group), F32),
                pltpu.VMEM((layers - 1, n_tp, tok, group), BF16),
                pltpu.VMEM((layers - 1, n_tp, tok, group), BF16),
                pltpu.VMEM((layers, tok, channels), BF16),
                pltpu.VMEM((tok, LANES), F32),
                pltpu.VMEM((kinds, 8, tok), F32),
                pltpu.VMEM((kinds, n_tp, 8, tok), F32),
                pltpu.VMEM((layers, HALO, group), BF16),
                pltpu.VMEM((layers, HALO, group), BF16),
                pltpu.VMEM((HALO + tok, group), F32),
                dma((mats, 2, reach)),
                dma((mats,)),
                dma((mats,)),
                dma((mats,)),
                dma((mats,)),
                dma((2,)),
                dma((6,)),
                dma((6,)),
                dma((layers - 1, n_tp)),
                dma((layers - 1, n_tp)),
                dma((kinds, n_tp)),
                dma((kinds, n_tp)),
                dma((layers, n_tp)),
                dma((layers, n_tp)),
                dma((layers,)),
                dma((layers,)),
            ],
            compiler_params=pltpu.CompilerParams(
                collective_id=0, has_side_effects=True, vmem_limit_bytes=60 * 1024 * 1024
            ),
        )(stream, gain_pre, w_in, w_pool, pool_scale, w_out, gain_post)

    return jax.shard_map(
        per_device,
        mesh=mesh,
        in_specs=(
            P(("grp", "sp"), "tp"),
            P(),
            P(None, "sp", "tp"),
            P(None, "tp", None, None),
            P(None, "tp"),
            P(None, "tp", "sp"),
            P(),
        ),
        out_specs=P(("grp", "sp"), "tp"),
        check_vma=False,
    )
```
